32 devices in a mesh: fs: 8 (over z, y), tp: 4 (over x, core).
Axes of the slice: x: 2, y: 2, z: 4, core: 2. Of those that a mesh axis runs over, the one named last changes fastest.
Arguments:
- tokens: bfloat16 [4096, 2048], P(('fs', 'tp')), may hold values from -6 to 6
- norm_gain: float32 [2048], replicated, may hold values from 0.1 to 1.9
- up_weight: float32 [2048, 8192], P('fs', 'tp'), may hold values from -0.125 to 0.125
- down_weight: float32 [8192, 2048], P('tp', 'fs'), may hold values from -0.0625 to 0.0625
Outputs:
- mlp_out: bfloat16 [4096, 2048], P(('fs', 'tp'))
The draws below stay inside these ranges and needn't reach their ends.
All inputs are finite; a program needn't handle non-finite values.
Results may differ from the reference program's by a relative error of at most 0.0017.
Values may be sent and summed in bfloat16 or wider, within the bound.
A program may use at most 64 MiB of HBM per device.

```python
import jax
import jax.numpy as jnp
from jax import lax

D = 2048
FF = 8192
TOKENS = 4096


def levels(rng, shape, pieces, least, largest):
    level = 1.0
    for axis_at, shards_of in pieces:
        steps = jax.random.uniform(jax.random.fold_in(jax.random.fold_in(rng, 6), axis_at), (shards_of,), jnp.float32, least / len(pieces), largest / len(pieces))
        level = level * jnp.repeat(jnp.exp(steps), shape[axis_at] // shards_of).reshape((-1,) + (1,) * (len(shape) - 1 - axis_at))
    return level


def noise(rng, extent, width, bound, cuts=(), held_as=jnp.bfloat16):
    entries = jax.random.normal(rng, extent, jnp.float32) * width
    if len(cuts) > 0:
        entries = levels(rng, extent, cuts, -0.22, 0.18) * entries
    return jnp.clip(entries, min=-bound, max=bound).astype(held_as)


def setup_inputs(seed: int = 0) -> dict:
    streams_of = jax.random.split(jax.random.key(seed), 5)
    return {
        "tokens": noise(streams_of[0], (TOKENS, D), 1.0, 6.0, ((0, 32),)),
        "norm_gain": jnp.clip(1.0 + 0.18 * jax.random.normal(streams_of[1], (D,), jnp.float32), 0.1, 1.9),
        "up_weight": noise(streams_of[2], (D, FF), D ** -0.5, 0.125, ((0, 8), (1, 4)), jnp.float32),
        "down_weight": noise(streams_of[3], (FF, D), FF ** -0.5, 0.0625, ((0, 4), (1, 8)), jnp.float32),
    }


epsilon = 1e-06

def reference(tokens, norm_gain, up_weight, down_weight):
    up_low = up_weight.astype(jnp.bfloat16)
    down_low = down_weight.astype(jnp.bfloat16)
    block_rows = min(TOKENS, 1024)
    blocks = tokens.reshape(TOKENS // block_rows, block_rows, D)

    def one_block(rows):
        values = rows.astype(jnp.float32)
        scale = lax.rsqrt(lax.optimization_barrier(jnp.mean(values * values, axis=-1, keepdims=True)) + epsilon)
        normed = (values * scale * norm_gain).astype(jnp.bfloat16)
        pre = jnp.dot(normed, up_low, preferred_element_type=jnp.float32)
        hidden = jnp.square(jax.nn.relu(pre)).astype(jnp.bfloat16)
        return jnp.dot(hidden, down_low, preferred_element_type=jnp.float32).astype(jnp.bfloat16)
    return lax.map(one_block, blocks).reshape(TOKENS, D)
```

```python
import functools

import jax
import jax.numpy as jnp
from jax import lax
from jax.experimental import pallas as pl
from jax.experimental.pallas import tpu as pltpu
from jax.sharding import PartitionSpec as P

epsilon = 1e-06
MESH = pl.DeviceIdType.MESH
VMEM_LIMIT = 66_000_000


def shards(tokens, norm_gain, up_weight, down_weight):
    values = tokens.astype(jnp.float32)
    scale = lax.rsqrt(jnp.mean(values * values, axis=-1, keepdims=True) + epsilon)
    normed = (values * scale * norm_gain).astype(jnp.bfloat16)
    grouped = lax.all_gather(normed, "tp", axis=0, tiled=True)
    up = lax.all_gather(up_weight.astype(jnp.bfloat16), "fs", axis=0, tiled=True)
    pre = jnp.dot(grouped, up, preferred_element_type=jnp.float32)
    hidden = jnp.square(jax.nn.relu(pre)).astype(jnp.bfloat16)
    down = lax.all_gather(down_weight.astype(jnp.bfloat16), "fs", axis=1, tiled=True)
    terms = jnp.dot(hidden, down, preferred_element_type=jnp.float32)
    summed = lax.psum_scatter(terms, "tp", scatter_dimension=0, tiled=True)
    return summed.astype(jnp.bfloat16)


def kernel(
    nz, ny, nx, nc,
    tok_ref, gain_ref, up_ref, down_ref, out_ref,
    tok, up, down, up_out, down_out, hidden, own, s1, r1, s2, r2,
    tok_recv, tok_send, tok_pass, up_recv, up_send, up_cross, down_recv, down_send, down_cross,
    s1_send, r1_recv, s2_send, r2_recv,
):
    chips = ny * nx
    fs, tp = lax.axis_index("fs"), lax.axis_index("tp")
    z, y = fs // ny, lax.rem(fs, ny)
    x, c = tp // nc, lax.rem(tp, nc)
    other = 1 - c
    me = y * nx + x
    part = up.shape[2]
    width = down.shape[2]

    def at(zz, yy, xx, cc):
        return (zz * ny + yy, xx * nc + cc)

    def chip(step):
        place = lax.rem(me + step, chips)
        return place, place // nx, lax.rem(place, nx)

    def remote(src, dst, send, recv, to):
        return pltpu.make_async_remote_copy(
            src_ref=src, dst_ref=dst, send_sem=send, recv_sem=recv, device_id=to, device_id_type=MESH
        )

    barrier = pltpu.get_barrier_semaphore()

    def greet(to):
        pl.semaphore_signal(barrier, inc=1, device_id=to, device_id_type=MESH)

    for step in range(1, chips):
        _, yy, xx = chip(step)
        greet(at(z, yy, xx, c))
    greet(at(z, y, x, other))
    pl.when(z > 0)(lambda: greet(at(z - 1, y, x, c)))
    pl.when(z < nz - 1)(lambda: greet(at(z + 1, y, x, c)))

    mine = z * ny + y
    up[mine] = up_ref[:, pl.ds(pl.multiple_of(y * part, 128), part)].astype(jnp.bfloat16)
    for step in range(1, ny):
        yy = lax.rem(y + step, ny)
        up_out[step - 1] = up_ref[:, pl.ds(pl.multiple_of(yy * part, 128), part)].astype(jnp.bfloat16)
    values = tok_ref[...].astype(jnp.float32)
    scale = lax.rsqrt(jnp.mean(values * values, axis=-1, keepdims=True) + epsilon)
    tok[c * chips + me] = (values * scale * gain_ref[...]).astype(jnp.bfloat16)

    pl.semaphore_wait(
        barrier, chips + (z > 0).astype(jnp.int32) + (z < nz - 1).astype(jnp.int32)
    )

    def along(buf, send, recv, slot, step):
        to = z + step
        side = (step + 1) // 2
        return remote(buf.at[slot], buf.at[slot], send.at[slot, side], recv.at[slot], at(to, y, x, c))

    def pass_on(buf, send, recv, zz, slot, wait=False):
        def go(step):
            copy = along(buf, send, recv, slot, step)
            copy.wait_send() if wait else copy.start()

        pl.when((zz <= z) & (z < nz - 1))(lambda: go(1))
        pl.when((zz >= z) & (z > 0))(lambda: go(-1))

    def arrive(buf, send, recv, slot):
        along(buf, send, recv, slot, 1).wait_recv()

    def cross(buf, dst, send, recv, step):
        yy = lax.rem(y + step, ny)
        return remote(buf.at[step - 1], dst.at[mine], send.at[step - 1], recv.at[mine], at(z, yy, x, c))

    pass_on(up, up_send, up_recv, z, mine)
    for step in range(1, ny):
        cross(up_out, up, up_cross, up_recv, step).start()

    def tok_to(step):
        _, yy, xx = chip(step)
        slot = tok.at[c * chips + me]
        return remote(slot, slot, tok_send.at[step - 1], tok_recv.at[c * chips + me], at(z, yy, xx, c))

    def tok_over(place):
        slot = tok.at[c * chips + place]
        return remote(
            slot, slot, tok_pass.at[place], tok_recv.at[c * chips + place], at(z, y, x, other)
        )

    for step in range(1, chips):
        tok_to(step).start()
    tok_over(me).start()

    down[mine] = down_ref[pl.ds(pl.multiple_of(y * part, 128), part), :].astype(jnp.bfloat16)
    for step in range(1, ny):
        yy = lax.rem(y + step, ny)
        down_out[step - 1] = down_ref[pl.ds(pl.multiple_of(yy * part, 128), part), :].astype(jnp.bfloat16)
    for step in range(1, ny):
        cross(down_out, down, down_cross, down_recv, step).start()

    def rounds(count):
        return [(0, 0)] + [(d, s) for d in range(1, count) for s in (-1, 1)]

    for number, (distance, side) in enumerate(rounds(nz)):
        zz = z + side * distance

        @pl.when((zz >= 0) & (zz < nz))
        def _():
            for step in range(ny):
                slot = zz * ny + lax.rem(y + step, ny)
                if distance > 0 or step > 0:
                    arrive(up, up_send, up_recv, slot)
                    pass_on(up, up_send, up_recv, zz, slot)

        if number == 2:
            for step in range(1, chips):
                place, _, _ = chip(step)
                slot = tok.at[c * chips + place]
                remote(slot, slot, tok_send.at[step - 1], tok_recv.at[c * chips + place], at(z, y, x, other)).wait_recv()
                tok_over(place).start()

    pass_on(down, down_send, down_recv, z, mine)
    for step in range(1, ny):
        slot = z * ny + lax.rem(y + step, ny)
        arrive(down, down_send, down_recv, slot)
        pass_on(down, down_send, down_recv, z, slot)
    for place in range(chips):
        slot = tok.at[other * chips + place]
        remote(
            slot, slot, tok_pass.at[place], tok_recv.at[other * chips + place], at(z, y, x, other)
        ).wait_recv()

    rows = tok.shape[0] * tok.shape[1]
    depth = tok.shape[2]
    tile = 256

    def hide(n, carry):
        columns = pl.ds(pl.multiple_of(n * tile, tile), tile)
        pre = jnp.dot(
            tok[...].reshape(rows, depth),
            up[:, :, columns].reshape(depth, tile),
            preferred_element_type=jnp.float32,
        )
        hidden[:, columns] = jnp.square(jnp.maximum(pre, 0.0)).astype(jnp.bfloat16)
        return carry

    lax.fori_loop(0, part // tile, hide, 0)

    half = rows // nc
    shard = half // chips

    def to_core(slot):
        return remote(s1.at[slot], r1.at[slot], s1_send.at[slot], r1_recv.at[slot], at(z, y, x, other))

    def to_chip(slot, step):
        place, yy, xx = chip(step)
        return remote(
            s2.at[slot, place], r2.at[slot, step - 1], s2_send.at[slot, step - 1],
            r2_recv.at[slot, step - 1], at(z, yy, xx, c),
        )

    def project(zz, step):
        slot = zz * ny + lax.rem(y + step, ny)

        @pl.when(zz != z)
        def _():
            arrive(down, down_send, down_recv, slot)
            pass_on(down, down_send, down_recv, zz, slot)

        theirs = hidden[pl.ds(pl.multiple_of(other * half, half), half), :]
        s1[slot] = jnp.dot(theirs, down[slot], preferred_element_type=jnp.float32)
        to_core(slot).start()
        ours = hidden[pl.ds(pl.multiple_of(c * half, half), half), :]
        own[...] = jnp.dot(ours, down[slot], preferred_element_type=jnp.float32)
        to_core(slot).wait_recv()
        s2[slot] = (own[...] + r1[slot]).reshape(chips, shard, width)
        for hop in range(1, chips):
            to_chip(slot, hop).start()

    def take(number, carry):
        turn, step = number // ny, lax.rem(number, ny)
        distance = (turn + 1) // 2
        zz = jnp.where(lax.rem(turn, 2) == 1, z - distance, z + distance)
        pl.when((zz >= 0) & (zz < nz))(lambda: project(zz, step))
        return carry

    lax.fori_loop(0, (2 * nz - 1) * ny, take, 0)

    def finish(number, carry):
        turn, step = number // ny, lax.rem(number, ny)
        distance = (turn + 1) // 2
        zz = jnp.where(lax.rem(turn, 2) == 1, z - distance, z + distance)

        @pl.when((zz >= 0) & (zz < nz))
        def _():
            slot = zz * ny + lax.rem(y + step, ny)
            total = s2[slot, me]
            for hop in range(1, chips):
                to_chip(slot, hop).wait_recv()
                total = total + r2[slot, hop - 1]
            out_ref[:, pl.ds(pl.multiple_of(slot * width, 128), width)] = total.astype(jnp.bfloat16)
            to_core(slot).wait_send()
            for hop in range(1, chips):
                to_chip(slot, hop).wait_send()
            pass_on(up, up_send, up_recv, zz, slot, wait=True)
            pass_on(down, down_send, down_recv, zz, slot, wait=True)

        return carry

    lax.fori_loop(0, (2 * nz - 1) * ny, finish, 0)

    for step in range(1, ny):
        cross(up_out, up, up_cross, up_recv, step).wait_send()
        cross(down_out, down, down_cross, down_recv, step).wait_send()
    for step in range(1, chips):
        tok_to(step).wait_send()
    for place in range(chips):
        tok_over(place).wait_send()


def solution(mesh):
    fs, tp = mesh.shape["fs"], mesh.shape["tp"]
    ny = 1
    while (2 * ny) * (2 * ny) <= fs and fs % (2 * ny) == 0:
        ny *= 2
    nz, nc = fs // ny, 2
    nx = tp // nc
    chips = ny * nx
    placed = (P(("fs", "tp"), None), P(), P("fs", "tp"), P("tp", "fs"))

    def whole(tokens, norm_gain, up_weight, down_weight):
        rows, depth = tokens.shape
        share, span = up_weight.shape
        part, width = span // ny, down_weight.shape[1]
        held = chips * nc
        half = chips * rows
        vm, dma = pltpu.VMEM, pltpu.SemaphoreType.DMA
        low, full = jnp.bfloat16, jnp.float32
        shapes = [
            ((held, rows, depth), low), ((fs, share, part), low), ((fs, part, width), low),
            ((ny - 1, share, part), low), ((ny - 1, part, width), low), ((held * rows, part), low),
            ((half, width), full), ((fs, half, width), full), ((fs, half, width), full),
            ((fs, chips, rows, width), full), ((fs, chips - 1, rows, width), full),
        ]
        size = 0
        for shape, kind in shapes:
            count = 4 if kind == full else 2
            for extent in shape:
                count *= extent
            size += count
        size += 4 * (up_weight.size + down_weight.size) + 4 * tokens.size
        if size > VMEM_LIMIT * 9 // 10 or part % 256 or tp % nc or ny < 2 or chips < 2:
            return shards(tokens, norm_gain, up_weight, down_weight)
        at_vmem = pl.BlockSpec(memory_space=pltpu.VMEM)
        return pl.pallas_call(
            functools.partial(kernel, nz, ny, nx, nc),
            out_shape=jax.ShapeDtypeStruct((rows, depth), jnp.bfloat16),
            in_specs=[at_vmem] * 4,
            out_specs=at_vmem,
            scratch_shapes=[vm(shape, kind) for shape, kind in shapes] + [
                dma((held,)), dma((chips - 1,)), dma((chips,)),
                dma((fs,)), dma((fs, 2)), dma((ny - 1,)),
                dma((fs,)), dma((fs, 2)), dma((ny - 1,)),
                dma((fs,)), dma((fs,)), dma((fs, chips - 1)), dma((fs, chips - 1)),
            ],
            compiler_params=pltpu.CompilerParams(
                collective_id=0, has_side_effects=True, vmem_limit_bytes=VMEM_LIMIT
            ),
        )(tokens, norm_gain.reshape(1, depth), up_weight, down_weight)

    return jax.shard_map(
        whole, mesh=mesh, in_specs=placed, out_specs=P(("fs", "tp"), None), check_vma=False
    )
```

```python
import functools

import jax
import jax.numpy as jnp
from jax import lax
from jax.experimental import pallas as pl
from jax.experimental.pallas import tpu as pltpu
from jax.sharding import PartitionSpec as P

epsilon = 1e-06
MESH = pl.DeviceIdType.MESH
VMEM_LIMIT = 66_000_000


def shards(tokens, norm_gain, up_weight, down_weight):
    values = tokens.astype(jnp.float32)
    scale = lax.rsqrt(jnp.mean(values * values, axis=-1, keepdims=True) + epsilon)
    normed = (values * scale * norm_gain).astype(jnp.bfloat16)
    grouped = lax.all_gather(normed, "tp", axis=0, tiled=True)
    up = lax.all_gather(up_weight.astype(jnp.bfloat16), "fs", axis=0, tiled=True)
    pre = jnp.dot(grouped, up, preferred_element_type=jnp.float32)
    hidden = jnp.square(jax.nn.relu(pre)).astype(jnp.bfloat16)
    down = lax.all_gather(down_weight.astype(jnp.bfloat16), "fs", axis=1, tiled=True)
    terms = jnp.dot(hidden, down, preferred_element_type=jnp.float32)
    summed = lax.psum_scatter(terms, "tp", scatter_dimension=0, tiled=True)
    return summed.astype(jnp.bfloat16)


def kernel(
    nz, ny, nx, nc, cuts,
    tok_ref, gain_ref, up_ref, down_ref, out_ref,
    tok, up, down, up_out, down_out, hidden, own, s1, r1, s2, r2,
    tok_recv, tok_send, tok_pass, up_recv, up_send, up_cross, down_recv, down_send, down_cross,
    s1_send, r1_recv, s2_send, r2_recv,
):
    chips = ny * nx
    fs, tp = lax.axis_index("fs"), lax.axis_index("tp")
    z, y = fs // ny, lax.rem(fs, ny)
    x, c = tp // nc, lax.rem(tp, nc)
    other = 1 - c
    me = y * nx + x
    part = up.shape[2]
    width = down.shape[2]
    whole = width * cuts
    outer = (z == 0) | (z == nz - 1)

    def at(zz, yy, xx, cc):
        return (zz * ny + yy, xx * nc + cc)

    def chip(step):
        place = lax.rem(me + step, chips)
        return place, place // nx, lax.rem(place, nx)

    def remote(src, dst, send, recv, to):
        return pltpu.make_async_remote_copy(
            src_ref=src, dst_ref=dst, send_sem=send, recv_sem=recv, device_id=to, device_id_type=MESH
        )

    barrier = pltpu.get_barrier_semaphore()

    def greet(to):
        pl.semaphore_signal(barrier, inc=1, device_id=to, device_id_type=MESH)

    for step in range(1, chips):
        _, yy, xx = chip(step)
        greet(at(z, yy, xx, c))
    greet(at(z, y, x, other))
    pl.when(z > 0)(lambda: greet(at(z - 1, y, x, c)))
    pl.when(z < nz - 1)(lambda: greet(at(z + 1, y, x, c)))

    mine = z * ny + y
    up[mine] = up_ref[:, pl.ds(pl.multiple_of(y * part, 128), part)].astype(jnp.bfloat16)
    for step in range(1, ny):
        yy = lax.rem(y + step, ny)
        up_out[step - 1] = up_ref[:, pl.ds(pl.multiple_of(yy * part, 128), part)].astype(jnp.bfloat16)
    pl.semaphore_wait(
        barrier, chips + (z > 0).astype(jnp.int32) + (z < nz - 1).astype(jnp.int32)
    )

    def along(buf, send, recv, slot, step):
        to = z + step
        side = (step + 1) // 2
        return remote(buf.at[slot], buf.at[slot], send.at[slot, side], recv.at[slot], at(to, y, x, c))

    def pass_on(buf, send, recv, zz, slot, wait=False):
        def go(step):
            copy = along(buf, send, recv, slot, step)
            copy.wait_send() if wait else copy.start()

        pl.when((zz <= z) & (z < nz - 1))(lambda: go(1))
        pl.when((zz >= z) & (z > 0))(lambda: go(-1))

    def arrive(buf, send, recv, slot):
        along(buf, send, recv, slot, 1).wait_recv()

    def cross(buf, dst, send, recv, step):
        yy = lax.rem(y + step, ny)
        return remote(buf.at[step - 1], dst.at[mine], send.at[step - 1], recv.at[mine], at(z, yy, x, c))

    def cross_down(step, cut):
        yy = lax.rem(y + step, ny)
        at_cut, to_cut = (step - 1) * cuts + cut, mine * cuts + cut
        return remote(
            down_out.at[at_cut], down.at[to_cut], down_cross.at[at_cut], down_recv.at[to_cut], at(z, yy, x, c)
        )

    def pass_down(slot):
        for cut in range(cuts):
            pass_on(down, down_send, down_recv, z, slot * cuts + cut)

    pass_on(up, up_send, up_recv, z, mine)
    for step in range(1, ny):
        cross(up_out, up, up_cross, up_recv, step).start()

    values = tok_ref[...].astype(jnp.float32)
    scale = lax.rsqrt(jnp.mean(values * values, axis=-1, keepdims=True) + epsilon)
    tok[c * chips + me] = (values * scale * gain_ref[...]).astype(jnp.bfloat16)
    for step in range(ny):
        yy = lax.rem(y + step, ny)
        for cut in range(cuts):
            piece = down_ref[
                pl.ds(pl.multiple_of(yy * part, 128), part), cut * width:(cut + 1) * width
            ].astype(jnp.bfloat16)
            if step == 0:
                down[mine * cuts + cut] = piece
            else:
                down_out[(step - 1) * cuts + cut] = piece

    def tok_to(step):
        _, yy, xx = chip(step)
        slot = tok.at[c * chips + me]
        return remote(slot, slot, tok_send.at[step - 1], tok_recv.at[c * chips + me], at(z, yy, xx, c))

    def tok_over(place):
        slot = tok.at[c * chips + place]
        return remote(
            slot, slot, tok_pass.at[place], tok_recv.at[c * chips + place], at(z, y, x, other)
        )

    for step in range(1, chips):
        tok_to(step).start()
    tok_over(me).start()
    pass_down(mine)
    for step in range(1, ny):
        for cut in range(cuts):
            cross_down(step, cut).start()

    def take_crossed():
        for step in range(1, ny):
            slot = z * ny + lax.rem(y + step, ny)
            for cut in range(cuts):
                arrive(down, down_send, down_recv, slot * cuts + cut)
            pass_down(slot)

    def rounds(count):
        return [(0, 0)] + [(d, s) for d in range(1, count) for s in (-1, 1)]

    for number, (distance, side) in enumerate(rounds(nz)):
        zz = z + side * distance

        @pl.when((zz >= 0) & (zz < nz))
        def _():
            for step in range(ny):
                slot = zz * ny + lax.rem(y + step, ny)
                if distance > 0 or step > 0:
                    arrive(up, up_send, up_recv, slot)
                    pass_on(up, up_send, up_recv, zz, slot)

        if number == 2:
            for step in range(1, chips):
                place, _, _ = chip(step)
                slot = tok.at[c * chips + place]
                remote(slot, slot, tok_send.at[step - 1], tok_recv.at[c * chips + place], at(z, y, x, other)).wait_recv()
                tok_over(place).start()
            pl.when(outer)(take_crossed)

    pl.when(~outer)(take_crossed)
    for place in range(chips):
        slot = tok.at[other * chips + place]
        remote(
            slot, slot, tok_pass.at[place], tok_recv.at[other * chips + place], at(z, y, x, other)
        ).wait_recv()

    rows = tok.shape[0] * tok.shape[1]
    depth = tok.shape[2]
    tile = 256

    def hide(n, carry):
        columns = pl.ds(pl.multiple_of(n * tile, tile), tile)
        pre = jnp.dot(
            tok[...].reshape(rows, depth),
            up[:, :, columns].reshape(depth, tile),
            preferred_element_type=jnp.float32,
        )
        hidden[:, columns] = jnp.square(jnp.maximum(pre, 0.0)).astype(jnp.bfloat16)
        return carry

    lax.fori_loop(0, part // tile, hide, 0)

    half = rows // nc
    shard = half // chips

    def to_core(slot):
        return remote(s1.at[slot], r1.at[slot], s1_send.at[slot], r1_recv.at[slot], at(z, y, x, other))

    def to_chip(slot, step):
        place, yy, xx = chip(step)
        return remote(
            s2.at[slot, place], r2.at[slot, step - 1], s2_send.at[slot, step - 1],
            r2_recv.at[slot, step - 1], at(z, yy, xx, c),
        )

    def blocks(number):
        turn, rest = number // (ny * cuts), lax.rem(number, ny * cuts)
        distance = (turn + 1) // 2
        zz = jnp.where(lax.rem(turn, 2) == 1, z - distance, z + distance)
        return zz, zz * ny + lax.rem(y + rest // cuts, ny), lax.rem(rest, cuts)

    def project(zz, slot):
        @pl.when(zz != z)
        def _():
            arrive(down, down_send, down_recv, slot)
            pass_on(down, down_send, down_recv, zz, slot)

        theirs = hidden[pl.ds(pl.multiple_of(other * half, half), half), :]
        s1[slot] = jnp.dot(theirs, down[slot], preferred_element_type=jnp.float32)
        to_core(slot).start()
        ours = hidden[pl.ds(pl.multiple_of(c * half, half), half), :]
        own[...] = jnp.dot(ours, down[slot], preferred_element_type=jnp.float32)
        to_core(slot).wait_recv()
        s2[slot] = (own[...] + r1[slot]).reshape(chips, shard, width)
        for hop in range(1, chips):
            to_chip(slot, hop).start()

    def take(number, carry):
        zz, slot, cut = blocks(number)
        pl.when((zz >= 0) & (zz < nz))(lambda: project(zz, slot * cuts + cut))
        return carry

    lax.fori_loop(0, (2 * nz - 1) * ny * cuts, take, 0)

    def finish(number, carry):
        zz, first, cut = blocks(number)

        @pl.when((zz >= 0) & (zz < nz))
        def _():
            slot = first * cuts + cut
            total = s2[slot, me]
            for hop in range(1, chips):
                to_chip(slot, hop).wait_recv()
                total = total + r2[slot, hop - 1]
            out_ref[:, pl.ds(pl.multiple_of(slot * width, 128), width)] = total.astype(jnp.bfloat16)
            to_core(slot).wait_send()
            for hop in range(1, chips):
                to_chip(slot, hop).wait_send()
            pass_on(down, down_send, down_recv, zz, slot, wait=True)
            pl.when(cut == 0)(lambda: pass_on(up, up_send, up_recv, zz, first, wait=True))

        return carry

    lax.fori_loop(0, (2 * nz - 1) * ny * cuts, finish, 0)

    for step in range(1, ny):
        cross(up_out, up, up_cross, up_recv, step).wait_send()
        for cut in range(cuts):
            cross_down(step, cut).wait_send()
    for step in range(1, chips):
        tok_to(step).wait_send()
    for place in range(chips):
        tok_over(place).wait_send()


def solution(mesh):
    fs, tp = mesh.shape["fs"], mesh.shape["tp"]
    ny = 1
    while (2 * ny) * (2 * ny) <= fs and fs % (2 * ny) == 0:
        ny *= 2
    nz, nc = fs // ny, 2
    nx = tp // nc
    chips, cuts = ny * nx, 2
    placed = (P(("fs", "tp"), None), P(), P("fs", "tp"), P("tp", "fs"))

    def whole(tokens, norm_gain, up_weight, down_weight):
        rows, depth = tokens.shape
        share, span = up_weight.shape
        part, width = span // ny, down_weight.shape[1] // cuts
        pieces = fs * cuts
        held = chips * nc
        half = chips * rows
        vm, dma = pltpu.VMEM, pltpu.SemaphoreType.DMA
        low, full = jnp.bfloat16, jnp.float32
        shapes = [
            ((held, rows, depth), low), ((fs, share, part), low), ((pieces, part, width), low),
            ((ny - 1, share, part), low), (((ny - 1) * cuts, part, width), low), ((held * rows, part), low),
            ((half, width), full), ((pieces, half, width), full), ((pieces, half, width), full),
            ((pieces, chips, rows, width), full), ((pieces, chips - 1, rows, width), full),
        ]
        size = 0
        for shape, kind in shapes:
            count = 4 if kind == full else 2
            for extent in shape:
                count *= extent
            size += count
        size += 4 * (up_weight.size + down_weight.size) + 4 * tokens.size
        if size > VMEM_LIMIT * 9 // 10 or part % 256 or width % 128 or tp % nc or ny < 2 or chips < 2:
            return shards(tokens, norm_gain, up_weight, down_weight)
        at_vmem = pl.BlockSpec(memory_space=pltpu.VMEM)
        return pl.pallas_call(
            functools.partial(kernel, nz, ny, nx, nc, cuts),
            out_shape=jax.ShapeDtypeStruct((rows, depth), jnp.bfloat16),
            in_specs=[at_vmem] * 4,
            out_specs=at_vmem,
            scratch_shapes=[vm(shape, kind) for shape, kind in shapes] + [
                dma((held,)), dma((chips - 1,)), dma((chips,)),
                dma((fs,)), dma((fs, 2)), dma((ny - 1,)),
                dma((pieces,)), dma((pieces, 2)), dma(((ny - 1) * cuts,)),
                dma((pieces,)), dma((pieces,)), dma((pieces, chips - 1)), dma((pieces, chips - 1)),
            ],
            compiler_params=pltpu.CompilerParams(
                collective_id=0, has_side_effects=True, vmem_limit_bytes=VMEM_LIMIT
            ),
        )(tokens, norm_gain.reshape(1, depth), up_weight, down_weight)

    return jax.shard_map(
        whole, mesh=mesh, in_specs=placed, out_specs=P(("fs", "tp"), None), check_vma=False
    )
```

```python
import functools

import jax
import jax.numpy as jnp
from jax import lax
from jax.experimental import pallas as pl
from jax.experimental.pallas import tpu as pltpu
from jax.sharding import PartitionSpec as P

epsilon = 1e-06
MESH = pl.DeviceIdType.MESH
VMEM_LIMIT = 66_000_000


def shards(tokens, norm_gain, up_weight, down_weight):
    values = tokens.astype(jnp.float32)
    scale = lax.rsqrt(jnp.mean(values * values, axis=-1, keepdims=True) + epsilon)
    normed = (values * scale * norm_gain).astype(jnp.bfloat16)
    grouped = lax.all_gather(normed, "tp", axis=0, tiled=True)
    up = lax.all_gather(up_weight.astype(jnp.bfloat16), "fs", axis=0, tiled=True)
    pre = jnp.dot(grouped, up, preferred_element_type=jnp.float32)
    hidden = jnp.square(jax.nn.relu(pre)).astype(jnp.bfloat16)
    down = lax.all_gather(down_weight.astype(jnp.bfloat16), "fs", axis=1, tiled=True)
    terms = jnp.dot(hidden, down, preferred_element_type=jnp.float32)
    summed = lax.psum_scatter(terms, "tp", scatter_dimension=0, tiled=True)
    return summed.astype(jnp.bfloat16)


def kernel(
    nz, ny, nx, nc, cuts,
    tok_ref, gain_ref, up_ref, down_ref, out_ref,
    tok, up, down, up_out, down_out, hidden, up_in, down_in, s1, r1, s2, r2,
    tok_recv, tok_send, tok_pass, up_recv, up_send, up_cross, down_recv, down_send, down_cross,
    s1_send, r1_recv, s2_send, r2_recv, load,
):
    chips = ny * nx
    fs, tp = lax.axis_index("fs"), lax.axis_index("tp")
    z, y = fs // ny, lax.rem(fs, ny)
    x, c = tp // nc, lax.rem(tp, nc)
    other = 1 - c
    me = y * nx + x
    part = up.shape[2]
    width = down.shape[2]
    outer = (z == 0) | (z == nz - 1)

    def at(zz, yy, xx, cc):
        return (zz * ny + yy, xx * nc + cc)

    def chip(step):
        place = lax.rem(me + step, chips)
        return place, place // nx, lax.rem(place, nx)

    def remote(src, dst, send, recv, to):
        return pltpu.make_async_remote_copy(
            src_ref=src, dst_ref=dst, send_sem=send, recv_sem=recv, device_id=to, device_id_type=MESH
        )

    barrier = pltpu.get_barrier_semaphore()

    def greet(to):
        pl.semaphore_signal(barrier, inc=1, device_id=to, device_id_type=MESH)

    for step in range(1, chips):
        _, yy, xx = chip(step)
        greet(at(z, yy, xx, c))
    greet(at(z, y, x, other))
    pl.when(z > 0)(lambda: greet(at(z - 1, y, x, c)))
    pl.when(z < nz - 1)(lambda: greet(at(z + 1, y, x, c)))

    mine = z * ny + y

    def piece_of(step):
        return pl.ds(pl.multiple_of(lax.rem(y + step, ny) * part, 128), part)

    def load_up(step):
        return pltpu.make_async_copy(
            up_ref.at[:, piece_of(step)], up_in.at[:, piece_of(step)], load.at[step]
        )

    load_down = pltpu.make_async_copy(down_ref, down_in, load.at[ny])
    for step in range(ny):
        load_up(step).start()
    load_down.start()
    for step in range(ny):
        load_up(step).wait()
        piece = up_in[:, piece_of(step)].astype(jnp.bfloat16)
        if step == 0:
            up[mine] = piece
        else:
            up_out[step - 1] = piece

    pl.semaphore_wait(
        barrier, chips + (z > 0).astype(jnp.int32) + (z < nz - 1).astype(jnp.int32)
    )

    def along(buf, send, recv, slot, step):
        to = z + step
        side = (step + 1) // 2
        return remote(buf.at[slot], buf.at[slot], send.at[slot, side], recv.at[slot], at(to, y, x, c))

    def pass_on(buf, send, recv, zz, slot, wait=False):
        def go(step):
            copy = along(buf, send, recv, slot, step)
            copy.wait_send() if wait else copy.start()

        pl.when((zz <= z) & (z < nz - 1))(lambda: go(1))
        pl.when((zz >= z) & (z > 0))(lambda: go(-1))

    def arrive(buf, send, recv, slot):
        along(buf, send, recv, slot, 1).wait_recv()

    def cross(buf, dst, send, recv, step):
        yy = lax.rem(y + step, ny)
        return remote(buf.at[step - 1], dst.at[mine], send.at[step - 1], recv.at[mine], at(z, yy, x, c))

    def cross_down(step, cut):
        yy = lax.rem(y + step, ny)
        at_cut, to_cut = (step - 1) * cuts + cut, mine * cuts + cut
        return remote(
            down_out.at[at_cut], down.at[to_cut], down_cross.at[at_cut], down_recv.at[to_cut], at(z, yy, x, c)
        )

    def pass_down(slot, first=0, last=cuts):
        for cut in range(first, last):
            pass_on(down, down_send, down_recv, z, slot * cuts + cut)

    pass_on(up, up_send, up_recv, z, mine)
    for step in range(1, ny):
        cross(up_out, up, up_cross, up_recv, step).start()

    values = tok_ref[...].astype(jnp.float32)
    scale = lax.rsqrt(jnp.mean(values * values, axis=-1, keepdims=True) + epsilon)
    tok[c * chips + me] = (values * scale * gain_ref[...]).astype(jnp.bfloat16)
    load_down.wait()
    for step in range(ny):
        for cut in range(cuts):
            piece = down_in[
                piece_of(step), cut * width:(cut + 1) * width
            ].astype(jnp.bfloat16)
            if step == 0:
                down[mine * cuts + cut] = piece
            else:
                down_out[(step - 1) * cuts + cut] = piece

    def tok_to(step):
        _, yy, xx = chip(step)
        slot = tok.at[c * chips + me]
        return remote(slot, slot, tok_send.at[step - 1], tok_recv.at[c * chips + me], at(z, yy, xx, c))

    def tok_over(place):
        slot = tok.at[c * chips + place]
        return remote(
            slot, slot, tok_pass.at[place], tok_recv.at[c * chips + place], at(z, y, x, other)
        )

    for step in range(1, chips):
        tok_to(step).start()
    tok_over(me).start()
    pass_down(mine)

    def take_crossed():
        for step in range(1, ny):
            slot = z * ny + lax.rem(y + step, ny)
            for cut in range(cuts):
                arrive(down, down_send, down_recv, slot * cuts + cut)
            pass_down(slot)

    def rounds(count):
        return [(0, 0)] + [(d, s) for d in range(1, count) for s in (-1, 1)]

    for number, (distance, side) in enumerate(rounds(nz)):
        zz = z + side * distance

        @pl.when((zz >= 0) & (zz < nz))
        def _():
            for step in range(ny):
                slot = zz * ny + lax.rem(y + step, ny)
                if distance > 0 or step > 0:
                    arrive(up, up_send, up_recv, slot)
                    pass_on(up, up_send, up_recv, zz, slot)

        if number == 0:
            for step in range(1, ny):
                for cut in range(cuts):
                    cross_down(step, cut).start()
        if number == 2:
            for step in range(1, chips):
                place, _, _ = chip(step)
                slot = tok.at[c * chips + place]
                remote(slot, slot, tok_send.at[step - 1], tok_recv.at[c * chips + place], at(z, y, x, other)).wait_recv()
                tok_over(place).start()
            pl.when(outer)(take_crossed)

    pl.when(~outer)(take_crossed)
    for place in range(chips):
        slot = tok.at[other * chips + place]
        remote(
            slot, slot, tok_pass.at[place], tok_recv.at[other * chips + place], at(z, y, x, other)
        ).wait_recv()

    rows = tok.shape[0] * tok.shape[1]
    depth = tok.shape[2]
    tile = 256

    def hide(n, carry):
        columns = pl.ds(pl.multiple_of(n * tile, tile), tile)
        pre = jnp.dot(
            tok[...].reshape(rows, depth),
            up[:, :, columns].reshape(depth, tile),
            preferred_element_type=jnp.float32,
        )
        hidden[:, columns] = jnp.square(jnp.maximum(pre, 0.0)).astype(jnp.bfloat16)
        return carry

    lax.fori_loop(0, part // tile, hide, 0)

    half = rows // nc
    shard = half // chips

    def to_core(slot):
        return remote(s1.at[slot], r1.at[slot], s1_send.at[slot], r1_recv.at[slot], at(z, y, x, other))

    def to_chip(slot, step):
        place, yy, xx = chip(step)
        return remote(
            s2.at[slot, place], r2.at[slot, step - 1], s2_send.at[slot, step - 1],
            r2_recv.at[slot, step - 1], at(z, yy, xx, c),
        )

    far = jnp.where(z >= nz // 2, -1, 1)
    reach = jnp.where(z >= nz // 2, z, nz - 1 - z)

    def blocks(number):
        turn, rest = number // (ny * cuts), lax.rem(number, ny * cuts)
        zz = z + jnp.where(turn <= reach, far * turn, far * (reach - turn))
        return zz, zz * ny + lax.rem(y + rest // cuts, ny), lax.rem(rest, cuts)

    def project(zz, slot):
        @pl.when((jnp.abs(zz - z) > 1) | (outer & (zz != z)))
        def _():
            arrive(down, down_send, down_recv, slot)
            pass_on(down, down_send, down_recv, zz, slot)

        theirs = hidden[pl.ds(pl.multiple_of(other * half, half), half), :]
        s1[slot] = jnp.dot(theirs, down[slot], preferred_element_type=jnp.float32)
        to_core(slot).start()
        ours = hidden[pl.ds(pl.multiple_of(c * half, half), half), :]
        s2[slot] = jnp.dot(ours, down[slot], preferred_element_type=jnp.float32).reshape(chips, shard, width)

    def spread(number):
        _, first, cut = blocks(number)
        slot = first * cuts + cut
        to_core(slot).wait_recv()
        s2[slot] = s2[slot] + r1[slot].reshape(chips, shard, width)
        for hop in range(1, chips):
            to_chip(slot, hop).start()

    def finish(number):
        _, first, cut = blocks(number)
        slot = first * cuts + cut
        total = s2[slot, me]
        for hop in range(1, chips):
            to_chip(slot, hop).wait_recv()
            total = total + r2[slot, hop - 1]
        out_ref[:, pl.ds(pl.multiple_of(slot * width, 128), width)] = total.astype(jnp.bfloat16)

    def hand_on(side):
        for piece in range(ny * cuts):
            slot = ((z + side) * ny + lax.rem(y + piece // cuts, ny)) * cuts + piece % cuts
            arrive(down, down_send, down_recv, slot)
            pass_on(down, down_send, down_recv, z + side, slot)

    @pl.when(~outer)
    def _():
        for side in (-1, 1):
            hand_on(side)

    steps, late = nz * ny * cuts, 4

    def take(number, carry):
        zz, slot, cut = blocks(number)
        project(zz, slot * cuts + cut)
        pl.when(number >= 1)(lambda: spread(number - 1))
        pl.when(number >= late)(lambda: finish(number - late))
        return carry

    lax.fori_loop(0, steps, take, 0)
    spread(steps - 1)

    def close(number, carry):
        finish(number)
        return carry

    lax.fori_loop(steps - late, steps, close, 0)

    def settle(number, carry):
        zz, first, cut = blocks(number)
        slot = first * cuts + cut
        to_core(slot).wait_send()
        for hop in range(1, chips):
            to_chip(slot, hop).wait_send()
        pass_on(down, down_send, down_recv, zz, slot, wait=True)
        pl.when(cut == 0)(lambda: pass_on(up, up_send, up_recv, zz, first, wait=True))
        return carry

    lax.fori_loop(0, steps, settle, 0)

    for step in range(1, ny):
        cross(up_out, up, up_cross, up_recv, step).wait_send()
        for cut in range(cuts):
            cross_down(step, cut).wait_send()
    for step in range(1, chips):
        tok_to(step).wait_send()
    for place in range(chips):
        tok_over(place).wait_send()


def solution(mesh):
    fs, tp = mesh.shape["fs"], mesh.shape["tp"]
    ny = 1
    while (2 * ny) * (2 * ny) <= fs and fs % (2 * ny) == 0:
        ny *= 2
    nz, nc = fs // ny, 2
    nx = tp // nc
    chips, cuts = ny * nx, 2
    placed = (P(("fs", "tp"), None), P(), P("fs", "tp"), P("tp", "fs"))

    def whole(tokens, norm_gain, up_weight, down_weight):
        rows, depth = tokens.shape
        share, span = up_weight.shape
        part, width = span // ny, down_weight.shape[1] // cuts
        pieces = fs * cuts
        held = chips * nc
        half = chips * rows
        vm, dma = pltpu.VMEM, pltpu.SemaphoreType.DMA
        low, full = jnp.bfloat16, jnp.float32
        shapes = [
            ((held, rows, depth), low), ((fs, share, part), low), ((pieces, part, width), low),
            ((ny - 1, share, part), low), (((ny - 1) * cuts, part, width), low), ((held * rows, part), low),
            ((share, span), full), ((span, width * cuts), full), ((pieces, half, width), full), ((pieces, half, width), full),
            ((pieces, chips, rows, width), full), ((pieces, chips - 1, rows, width), full),
        ]
        size = 0
        for shape, kind in shapes:
            count = 4 if kind == full else 2
            for extent in shape:
                count *= extent
            size += count
        size += 4 * tokens.size
        if size > VMEM_LIMIT * 9 // 10 or part % 256 or width % 128 or tp % nc or ny < 2 or chips < 2 or nz > 4:
            return shards(tokens, norm_gain, up_weight, down_weight)
        at_vmem = pl.BlockSpec(memory_space=pltpu.VMEM)
        return pl.pallas_call(
            functools.partial(kernel, nz, ny, nx, nc, cuts),
            out_shape=jax.ShapeDtypeStruct((rows, depth), jnp.bfloat16),
            in_specs=[at_vmem] * 2 + [pl.BlockSpec(memory_space=pl.ANY)] * 2,
            out_specs=at_vmem,
            scratch_shapes=[vm(shape, kind) for shape, kind in shapes] + [
                dma((held,)), dma((chips - 1,)), dma((chips,)),
                dma((fs,)), dma((fs, 2)), dma((ny - 1,)),
                dma((pieces,)), dma((pieces, 2)), dma(((ny - 1) * cuts,)),
                dma((pieces,)), dma((pieces,)), dma((pieces, chips - 1)), dma((pieces, chips - 1)), dma((ny + 1,)),
            ],
            compiler_params=pltpu.CompilerParams(
                collective_id=0, has_side_effects=True, vmem_limit_bytes=VMEM_LIMIT
            ),
        )(tokens, norm_gain.reshape(1, depth), up_weight, down_weight)

    return jax.shard_map(
        whole, mesh=mesh, in_specs=placed, out_specs=P(("fs", "tp"), None), check_vma=False
    )
```
